32 devices in a mesh: tp: 8 (over z, y), dp: 4 (over x, core).
Axes of the slice: x: 2, y: 2, z: 4, core: 2. Of those that a mesh axis runs over, the one named last changes fastest.
Arguments:
- stream: bfloat16 [128, 4096], P(None, ('dp', 'tp')), may hold values from -16 to 16
- lengths: int32 [128], P('dp'), may hold values from 1 to 64, 1024 in all
- prior_state: float32 [2, 128, 4096], P(None, 'dp', 'tp'), may hold values from -6 to 6
- prior_window: bfloat16 [2, 128, 3, 4096], P(None, 'dp', None, 'tp'), may hold values from -6 to 6
- norm_gain: float32 [2, 4096], P(None, 'dp'), may hold values from 0.1 to 1.9
- w_branch: bfloat16 [2, 4096, 4096], P(None, 'dp', 'tp'), may hold values from -0.09375 to 0.09375
- w_gate_branch: bfloat16 [2, 4096, 4096], P(None, 'dp', 'tp'), may hold values from -0.09375 to 0.09375
- conv_taps: bfloat16 [2, 4, 4096], P(None, None, 'tp'), may hold values from -3 to 3
- w_in_gate: bfloat16 [2, 256, 4096], P(None, None, 'tp'), may hold values from -0.375 to 0.375
- w_rec_gate: bfloat16 [2, 256, 4096], P(None, None, 'tp'), may hold values from -0.375 to 0.375
- decay_param: float32 [2, 4096], P(None, 'tp'), may hold values from -1 to 4
- w_out: bfloat16 [2, 4096, 4096], P(None, 'tp', 'dp'), may hold values from -0.1875 to 0.1875
Outputs:
- mixed_out: bfloat16 [128, 4096], P(None, ('dp', 'tp'))
- new_state: float32 [2, 128, 4096], P(None, 'dp', 'tp')
- new_window: bfloat16 [2, 128, 3, 4096], P(None, 'dp', None, 'tp')
The draws below stay inside these ranges and needn't reach their ends.
All inputs are finite; a program needn't handle non-finite values. No bound on the sum of `lengths` on one device may be relied on, other than what follows from the above.
Results may differ from the reference program's by a relative error of at most 0.014.
Values may be sent and summed in bfloat16 or wider, within the bound.
A program may use at most 64 MiB of HBM per device.

```python
import math
import jax
import jax.numpy as jnp
import numpy as np
from jax import lax

D = 4096
D_RNN = 4096
BLOCK = 256
TAPS = 4
LAYERS = 2
BATCH = 128
N_TP = 8
N_DP = 4


def draw_stream(key, part):
    feature = jnp.arange(D)
    per_device = D // (N_DP * N_TP)
    along_dp = (feature // (D // N_DP)).astype(jnp.float32) / max(N_DP - 1, 1)
    along_tp = (feature // per_device % N_TP).astype(jnp.float32) / max(N_TP - 1, 1)
    rising = jnp.exp(jnp.log(3.0) * (along_dp + along_tp))
    values = jax.random.normal(key, (BATCH, D), jnp.float32) * 0.4 * rising
    return jnp.clip(values, -16.0, 16.0).astype(jnp.bfloat16)


def strengthened(values, stream_key, source, target, shards_of, factor):
    def block_of(axis_at):
        return (jnp.arange(values.shape[axis_at]) // (values.shape[axis_at] // shards_of)).reshape((-1,) + (1,) * (values.ndim - 1 - axis_at))

    near = jax.random.permutation(stream_key, shards_of)[block_of(target)]
    far = (block_of(target) + shards_of // 2) % shards_of
    return jnp.where((block_of(source) == near) | (block_of(source) == far), factor * values, values)


def levels(own_key, dims, split, least, largest):
    def one(axis_at, shards_of):
        draws = jax.random.uniform(jax.random.fold_in(jax.random.fold_in(own_key, 6), axis_at), (shards_of,), jnp.float32, least / len(split), largest / len(split))
        return jnp.repeat(jnp.exp(draws), dims[axis_at] // shards_of).reshape((-1,) + (1,) * (len(dims) - axis_at - 1))

    loudness = one(*split[0])
    for cut in split[1:]:
        loudness = loudness * one(*cut)
    return loudness


def split_up(amount, total, most, lean):
    portions = [(1 << 20) // math.isqrt(standing ** lean) + 1 for standing in range(2, amount + 1)]
    surplus, holding = total - most - (amount - 1), [1] * (amount - 1)
    while surplus > 0:
        candidates = [i for i in range(amount - 1) if holding[i] < most]
        whole, left = sum([portions[i] for i in candidates]), surplus
        for i in candidates:
            addition = min(most - holding[i], max(1, left * portions[i] // whole), surplus)
            holding[i] = holding[i] + addition
            surplus = surplus - addition
    return np.array([most] + holding)


def ragged_sizes(key, count, total, reach, skew):
    if count == 2:
        one = jax.random.randint(key, (), max(1, total - reach), min(reach, total - 1) + 1)
        return jnp.stack([one, total - one])
    sizes = jnp.asarray(split_up(count, total, reach, skew), jnp.int32)
    twos = (count - 1) // 2
    giver, receiver = sizes[1:1 + 2 * twos:2], sizes[2:2 + 2 * twos:2]
    margin = jnp.minimum(giver - 1, reach - receiver)
    moved = jax.random.randint(jax.random.fold_in(key, 1), (twos,), 0, 1 << 20) % (margin + 1)
    sizes = sizes.at[1:1 + 2 * twos:2].set(giver - moved).at[2:2 + 2 * twos:2].set(receiver + moved)
    return sizes[jax.random.permutation(jax.random.fold_in(key, 2), count)]


def gaussian(stream_key, shape, deviation, reach, split=(), held_as=jnp.bfloat16):
    array = deviation * jax.random.normal(stream_key, shape, jnp.float32)
    if split:
        array = array * levels(stream_key, shape, split, -0.22, 0.18)
    return jnp.clip(array, -reach, reach).astype(held_as)


def heavy_noise(stream_key, extent, deviation, most, split, heavy, kind=jnp.bfloat16):
    values = deviation * jax.random.normal(stream_key, extent, jnp.float32)
    if split:
        values = values * levels(stream_key, extent, split, -0.22, 0.18)
    return jnp.clip(strengthened(values, jax.random.fold_in(stream_key, 3), *heavy), -most, most).astype(kind)


def setup_inputs(seed: int = 0) -> dict:
    arg_keys = jax.random.split(jax.random.key(seed), 13)
    stream = draw_stream(jax.random.fold_in(arg_keys[12], 71), 0)
    lengths = ragged_sizes(arg_keys[1], BATCH, 8 * BATCH, 64, 2).astype(jnp.int32)
    prior_state = gaussian(arg_keys[2], (LAYERS, BATCH, D_RNN), 1.0, 6.0, ((1, 4), (2, 8)), jnp.float32)
    prior_window = gaussian(arg_keys[3], (LAYERS, BATCH, TAPS - 1, D_RNN), 1.0, 6.0, ((1, 4), (3, 8)))
    norm_gain = jnp.clip(1.0 + 0.18 * jax.random.normal(arg_keys[4], (LAYERS, D), jnp.float32), 0.1, 1.9)
    w_branch = gaussian(arg_keys[5], (LAYERS, D, D_RNN), D ** -0.5, 0.09375, ((1, 4), (2, 8)))
    w_gate_branch = gaussian(arg_keys[6], (LAYERS, D, D_RNN), D ** -0.5, 0.09375, ((1, 4), (2, 8)))
    conv_taps = gaussian(arg_keys[7], (LAYERS, TAPS, D_RNN), TAPS ** -0.5, 3.0, ((2, 8),))
    w_in_gate = gaussian(arg_keys[8], (LAYERS, BLOCK, D_RNN), BLOCK ** -0.5, 0.375, ((2, 8),))
    w_rec_gate = gaussian(arg_keys[9], (LAYERS, BLOCK, D_RNN), BLOCK ** -0.5, 0.375, ((2, 8),))
    decay_param = jnp.clip(-1.0 + 5.0 * jax.random.uniform(arg_keys[10], (LAYERS, D_RNN), jnp.float32) ** levels(arg_keys[10], (LAYERS, D_RNN), ((1, 8),), -0.2, 0.2), -1.0, 4.0)
    w_out = heavy_noise(arg_keys[11], (LAYERS, D_RNN, D), (D_RNN // 2) ** -0.5, 0.1875, ((1, 8), (2, 4)), (1, 2, 8, 2.0))
    return {"stream": stream, "lengths": lengths, "prior_state": prior_state, "prior_window": prior_window, "norm_gain": norm_gain, "w_branch": w_branch, "w_gate_branch": w_gate_branch, "conv_taps": conv_taps, "w_in_gate": w_in_gate, "w_rec_gate": w_rec_gate, "decay_param": decay_param, "w_out": w_out}


epsilon = 1e-06

def block_map(convolved, weight):
    row_count = convolved.shape[0]
    blocks = D_RNN // BLOCK
    inputs = convolved.astype(jnp.float32).reshape(row_count, blocks, BLOCK)
    tables = weight.astype(jnp.float32).reshape(BLOCK, blocks, BLOCK)
    return jnp.einsum('rnk,knc->rnc', inputs, tables).reshape(row_count, D_RNN)

def projected(normed, weight):
    block_width = D // N_DP

    def add_block(running, index):
        offset = (index * block_width).astype(jnp.int32)
        columns = lax.dynamic_slice_in_dim(normed, offset, block_width, 1)
        weight_rows = lax.dynamic_slice_in_dim(weight, offset, block_width, 0)
        partial_sum = jnp.dot(columns, weight_rows, preferred_element_type=jnp.float32).astype(jnp.bfloat16)
        partial_sum = lax.optimization_barrier(partial_sum)
        return (running + partial_sum.astype(jnp.float32), None)
    start_sum = jnp.zeros((normed.shape[0], weight.shape[1]), jnp.float32)
    running, _ = lax.scan(add_block, start_sum, jnp.arange(N_DP, dtype=jnp.int32))
    return running.astype(jnp.bfloat16)

def recurrent_block(stream, lengths, prior_state, prior_window, norm_gain, w_branch, w_gate_branch, conv_taps, w_in_gate, w_rec_gate, decay_param, w_out):
    widened = stream.astype(jnp.float32)
    squares = lax.optimization_barrier(jnp.sum(widened * widened, axis=1, keepdims=True))
    normed = (widened * lax.rsqrt(squares / D + epsilon) * norm_gain).astype(jnp.bfloat16)
    branch = projected(normed, w_branch)
    gate_in = projected(normed, w_gate_branch)
    depth = prior_window.shape[1]
    needed = depth + 1 - jnp.arange(depth, dtype=jnp.int32)
    living = lengths[:, None, None] >= needed[None, :, None]
    history = jnp.where(living, prior_window, jnp.zeros_like(prior_window))
    window = jnp.concatenate([history, branch[:, None, :]], axis=1)
    convolved = lax.optimization_barrier(jnp.sum(window.astype(jnp.float32) * conv_taps.astype(jnp.float32)[None], axis=1)).astype(jnp.bfloat16)
    input_gate = jax.nn.sigmoid(block_map(convolved, w_in_gate))
    recur_gate = jax.nn.sigmoid(block_map(convolved, w_rec_gate))
    log_keep = 8.0 * recur_gate * jax.nn.log_sigmoid(decay_param)
    keeping = jnp.exp(log_keep)
    feeding = jnp.sqrt(-jnp.expm1(2.0 * log_keep))
    earlier = jnp.where(lengths[:, None] >= 2, prior_state, jnp.zeros_like(prior_state))
    state = keeping * earlier + feeding * input_gate * convolved.astype(jnp.float32)
    readout = (state * jax.nn.gelu(gate_in.astype(jnp.float32))).astype(jnp.bfloat16)
    result = (widened + jnp.dot(readout, w_out, preferred_element_type=jnp.float32)).astype(jnp.bfloat16)
    return (result, state, window[:, 1:])

def reference(stream, lengths, prior_state, prior_window, norm_gain, w_branch, w_gate_branch, conv_taps, w_in_gate, w_rec_gate, decay_param, w_out):
    first, state_first, window_first = recurrent_block(stream, lengths, prior_state[0], prior_window[0], norm_gain[0], w_branch[0], w_gate_branch[0], conv_taps[0], w_in_gate[0], w_rec_gate[0], decay_param[0], w_out[0])
    second, state_second, window_second = recurrent_block(first, lengths, prior_state[1], prior_window[1], norm_gain[1], w_branch[1], w_gate_branch[1], conv_taps[1], w_in_gate[1], w_rec_gate[1], decay_param[1], w_out[1])
    return (second, jnp.stack([state_first, state_second]), jnp.stack([window_first, window_second]))
```

```python
import functools

import jax
import jax.numpy as jnp
from jax import lax
from jax.experimental import pallas as pl
from jax.experimental.pallas import tpu as pltpu
from jax.sharding import PartitionSpec as P

D = 4096
BLOCK = 256


epsilon = 1e-06


def from_partner(block, axis, apart):
    count = lax.axis_size(axis)
    route = []
    for low in range(count):
        high = low | 1 << apart
        if high != low and high < count:
            route += [(low, high), (high, low)]
    return lax.ppermute(block, axis, route)


def norm_rows(block_rows, gain_values, squares):
    scaling = lax.rsqrt(squares / D + epsilon)
    return (block_rows.astype(jnp.float32) * scaling * gain_values).astype(jnp.bfloat16)


def normed_input(stream_local, gain_block):
    own_width = stream_local.shape[1]
    offset = lax.axis_index("tp") * own_width
    widened = stream_local.astype(jnp.float32)
    squares = lax.psum(jnp.sum(widened * widened, axis=1, keepdims=True), ("tp", "dp"))
    own_gain = lax.dynamic_slice_in_dim(gain_block, offset, own_width, 0)
    result = lax.all_gather(norm_rows(stream_local, own_gain, squares), "tp", axis=1, tiled=True)
    return result


def peer_block(convolved):
    col_count = convolved.shape[1]
    group_size = max(BLOCK // col_count, 1)
    device = lax.axis_index("tp")
    grouped = convolved
    for bit_number in range(group_size.bit_length() - 1):
        partner = from_partner(grouped, "tp", bit_number)
        is_upper = device // (1 << bit_number) % 2 == 1
        grouped = jnp.where(
            is_upper,
            jnp.concatenate([partner, grouped], axis=1),
            jnp.concatenate([grouped, partner], axis=1),
        )
    return grouped


def block_gates(grouped, weight):
    row_count = grouped.shape[0]
    col_count = weight.shape[1]
    blocks = max(col_count // BLOCK, 1)
    block_cols = min(col_count, BLOCK)
    inputs = grouped.reshape(row_count, blocks, BLOCK)
    tables = weight.reshape(BLOCK, blocks, block_cols)
    mapped = jnp.einsum("rnk,knc->rnc", inputs, tables, preferred_element_type=jnp.float32)
    return mapped.reshape(row_count, col_count)


def recurrent_step(
    normed,
    lengths,
    prior_state,
    prior_window,
    w_branch,
    w_gate_branch,
    conv_taps,
    w_in_gate,
    w_rec_gate,
    decay_param,
    w_out,
    stream_local,
):
    col_count = w_branch.shape[1]
    summed = lax.psum_scatter(
        jnp.concatenate(
            [
                jnp.dot(normed, w_branch, preferred_element_type=jnp.float32),
                jnp.dot(normed, w_gate_branch, preferred_element_type=jnp.float32),
            ],
            axis=1,
        ).astype(jnp.bfloat16),
        "dp",
        scatter_dimension=0,
        tiled=True,
    ).astype(jnp.float32)
    branch = summed[:, :col_count].astype(jnp.bfloat16)
    gate_in = summed[:, col_count:].astype(jnp.bfloat16)
    depth = prior_window.shape[1]
    needed = depth + 1 - jnp.arange(depth, dtype=jnp.int32)
    living = lengths[:, None, None] >= needed[None, :, None]
    history = jnp.where(living, prior_window, jnp.zeros_like(prior_window))
    window = jnp.concatenate([history, branch[:, None, :]], axis=1)
    convolved = jnp.sum(
        window.astype(jnp.float32) * conv_taps.astype(jnp.float32)[None], axis=1
    ).astype(jnp.bfloat16)
    grouped = peer_block(convolved)
    input_gate = jax.nn.sigmoid(block_gates(grouped, w_in_gate))
    recur_gate = jax.nn.sigmoid(block_gates(grouped, w_rec_gate))
    log_keep = 8.0 * recur_gate * jax.nn.log_sigmoid(decay_param)
    keeping = jnp.exp(log_keep)
    feeding = jnp.sqrt(-jnp.expm1(2.0 * log_keep))
    earlier = jnp.where(lengths[:, None] >= 2, prior_state, jnp.zeros_like(prior_state))
    state = keeping * earlier + feeding * input_gate * convolved.astype(jnp.float32)
    readout = (state * jax.nn.gelu(gate_in.astype(jnp.float32))).astype(jnp.bfloat16)
    mixed = jnp.dot(
        lax.all_gather(readout, "dp", axis=0, tiled=True), w_out, preferred_element_type=jnp.float32
    )
    own_width = stream_local.shape[1]
    offset = lax.axis_index("tp") * own_width
    own_cols = lax.dynamic_slice_in_dim(mixed, offset, own_width, 1) + stream_local.astype(
        jnp.float32
    )
    terms = lax.dynamic_update_slice_in_dim(mixed, own_cols, offset, 1)
    return (terms, state, window[:, 1:])


def body(
    stream,
    lengths,
    prior_state,
    prior_window,
    norm_gain,
    w_branch,
    w_gate_branch,
    conv_taps,
    w_in_gate,
    w_rec_gate,
    decay_param,
    w_out,
):
    normed = normed_input(stream, norm_gain[0])
    terms, state_first, window_first = recurrent_step(
        normed,
        lengths,
        prior_state[0],
        prior_window[0],
        w_branch[0],
        w_gate_branch[0],
        conv_taps[0],
        w_in_gate[0],
        w_rec_gate[0],
        decay_param[0],
        w_out[0],
        stream,
    )
    carried = lax.psum(terms, "tp").astype(jnp.bfloat16)
    widened = carried.astype(jnp.float32)
    squares = lax.psum(jnp.sum(widened * widened, axis=1, keepdims=True), "dp")
    normed = norm_rows(carried, norm_gain[1], squares)
    own_width = stream.shape[1]
    first = lax.dynamic_slice_in_dim(carried, lax.axis_index("tp") * own_width, own_width, 1)
    terms, state_second, window_second = recurrent_step(
        normed,
        lengths,
        prior_state[1],
        prior_window[1],
        w_branch[1],
        w_gate_branch[1],
        conv_taps[1],
        w_in_gate[1],
        w_rec_gate[1],
        decay_param[1],
        w_out[1],
        first,
    )
    second = lax.psum_scatter(terms, "tp", scatter_dimension=1, tiled=True).astype(jnp.bfloat16)
    return (
        second,
        jnp.stack([state_first, state_second]),
        jnp.stack([window_first, window_second]),
    )


HALVES = 2
MESH = pl.DeviceIdType.MESH


def negative_expm1(z):
    series = -z * (1.0 + z / 2.0 * (1.0 + z / 3.0 * (1.0 + z / 4.0 * (1.0 + z / 5.0))))
    return jnp.where(z > -0.1, series, 1.0 - jnp.exp(z))


def fused_kernel(
    nt,
    nd,
    halves,
    stream,
    lengths,
    prior_state,
    prior_window,
    norm_gain,
    w_branch,
    w_gate_branch,
    conv_taps,
    w_in_gate,
    w_rec_gate,
    decay_param,
    w_out,
    mixed_out,
    new_state,
    new_window,
    xg,
    part,
    pr,
    ro,
    rg,
    mx,
    ms,
    len_v,
    state_v,
    win_v,
    gain_v,
    wp_v,
    taps_v,
    gates_v,
    decay_v,
    wo_v,
    state_o,
    win_o,
    mix_o,
    in_sem,
    out_sem,
    xs,
    xr,
    ps,
    prs,
    gs,
    gr,
    ms_s,
    ms_r,
):
    t = lax.axis_index("tp")
    d = lax.axis_index("dp")
    layers = w_branch.shape[0]
    rows, own = stream.shape[1], stream.shape[2]
    r = rows // halves
    cols = w_branch.shape[2]
    width = w_branch.shape[1]

    barrier = pltpu.get_barrier_semaphore()
    tp_peers = [lax.rem(t + k, nt) for k in range(1, nt)]
    dp_peers = [lax.rem(d + k, nd) for k in range(1, nd)]
    for peer in tp_peers:
        pl.semaphore_signal(barrier, inc=1, device_id={"tp": peer}, device_id_type=MESH)
    for peer in dp_peers:
        pl.semaphore_signal(barrier, inc=1, device_id={"dp": peer}, device_id_type=MESH)

    counter = [0]

    def load(src, dst):
        copy = pltpu.make_async_copy(src, dst, in_sem.at[counter[0]])
        counter[0] += 1
        copy.start()
        return copy

    c_stream = load(stream, xg.at[0, t])
    c_gain = load(norm_gain, gain_v)
    c_len = load(lengths, len_v)
    loads = []
    for l in range(layers):
        c_w = [load(w_branch.at[l], wp_v.at[l, 0]), load(w_gate_branch.at[l], wp_v.at[l, 1])]
        c_s = [
            load(prior_window.at[l], win_v.at[l]),
            load(prior_state.at[l], state_v.at[l]),
            load(w_in_gate.at[l], gates_v.at[l, 0]),
            load(w_rec_gate.at[l], gates_v.at[l, 1]),
        ]
        if l == 0:
            c_s += [load(conv_taps, taps_v), load(decay_param, decay_v), c_len]
        c_o = [load(w_out.at[l], wo_v.at[l])]
        loads.append((c_w, c_s, c_o))

    sends = []

    def send(src, dst, ssem, rsem, axis, peer):
        copy = pltpu.make_async_remote_copy(
            src_ref=src,
            dst_ref=dst,
            send_sem=ssem,
            recv_sem=rsem,
            device_id={axis: peer},
            device_id_type=MESH,
        )
        copy.start()
        sends.append(copy)

    def arrived(dst, ssem, rsem, axis, peer):
        pltpu.make_async_remote_copy(
            src_ref=dst,
            dst_ref=dst,
            send_sem=ssem,
            recv_sem=rsem,
            device_id={axis: peer},
            device_id_type=MESH,
        ).wait_recv()

    def cut(h):
        return slice(h * r, (h + 1) * r)

    def send_features(l, h):
        for k, peer in enumerate(tp_peers):
            block = xg.at[l, t, :, pl.ds(h * r, r), :]
            send(block, block, xs.at[l, h, k], xr.at[l, h, t], "tp", peer)

    def project(l, h):
        for k, peer in enumerate(tp_peers):
            block = xg.at[l, peer, :, pl.ds(h * r, r), :]
            arrived(block, xs.at[l, h, k], xr.at[l, h, peer], "tp", peer)
        if h == 0:
            if l == 0:
                c_gain.wait()
            for copy in loads[l][0]:
                copy.wait()
        squares = jnp.zeros((nd * r, own), jnp.float32)
        pieces = []
        for j in range(nt):
            x = xg[l, j, :, cut(h), :].reshape(nd * r, own).astype(jnp.float32)
            squares = squares + x * x
            gain = gain_v[l : l + 1, j * own : (j + 1) * own]
            pieces.append((x * gain).astype(jnp.bfloat16))
        normed = jnp.concatenate(pieces, axis=1)
        total = jnp.sum(squares, axis=1, keepdims=True)
        high = total.astype(jnp.bfloat16).astype(jnp.float32)
        lane = lax.broadcasted_iota(jnp.int32, (nd * r, 128), 1)
        both = jnp.where(lane < 64, high, total - high).astype(jnp.bfloat16)
        part[l, h, :, :, 2 * cols :] = both.reshape(nd, r, 128)
        for w in range(2):
            product = jnp.dot(normed, wp_v[l, w], preferred_element_type=jnp.float32)
            part[l, h, :, :, w * cols : (w + 1) * cols] = product.astype(jnp.bfloat16).reshape(
                nd, r, cols
            )
        for k, peer in enumerate(dp_peers):
            send(
                part.at[l, h, peer],
                pr.at[l, h, d],
                ps.at[l, h, k],
                prs.at[l, h, d],
                "dp",
                peer,
            )

    def recur(l, h):
        summed = part[l, h, d].astype(jnp.float32)
        if h == 0:
            for copy in loads[l][1]:
                copy.wait()
        length = jnp.sum(
            jnp.where(
                lax.broadcasted_iota(jnp.int32, (r, rows), 0) + h * r
                == lax.broadcasted_iota(jnp.int32, (r, rows), 1),
                jnp.broadcast_to(len_v[...].astype(jnp.float32), (r, rows)),
                0.0,
            ),
            axis=1,
            keepdims=True,
        )
        depth = prior_window.shape[1]
        history = []
        for m in range(depth):
            row = win_v[l, m, cut(h), :].astype(jnp.float32)
            history.append(jnp.where(length >= depth + 1 - m, row, 0.0))
        taps = taps_v[l].astype(jnp.float32)
        before = history[0] * taps[0:1]
        for m in range(1, depth):
            before = before + history[m] * taps[m : m + 1]
        raw = decay_v[l : l + 1]
        log_decay = jnp.minimum(raw, 0.0) - jnp.log1p(jnp.exp(-jnp.abs(raw)))
        earlier = jnp.where(length >= 2, state_v[l, cut(h), :], 0.0)

        for k, peer in enumerate(dp_peers):
            arrived(pr.at[l, h, peer], ps.at[l, h, k], prs.at[l, h, peer], "dp", peer)
        for peer in dp_peers:
            summed = summed + pr[l, h, peer].astype(jnp.float32)
        squares = summed[:, 2 * cols : 2 * cols + 1] + summed[:, 2 * cols + 64 : 2 * cols + 65]
        scaling = lax.rsqrt(squares / (width * nd) + epsilon)
        branch = (summed[:, :cols] * scaling).astype(jnp.bfloat16)
        gate_in = (summed[:, cols : 2 * cols] * scaling).astype(jnp.bfloat16)
        for m in range(1, depth):
            win_o[l, m - 1, cut(h), :] = history[m].astype(jnp.bfloat16)
        win_o[l, depth - 1, cut(h), :] = branch
        convolved = (before + branch.astype(jnp.float32) * taps[depth : depth + 1]).astype(
            jnp.bfloat16
        )
        mapped = []
        for w in range(2):
            mapped.append(
                jnp.concatenate(
                    [
                        jnp.dot(
                            convolved[:, n * BLOCK : (n + 1) * BLOCK],
                            gates_v[l, w, :, n * BLOCK : (n + 1) * BLOCK],
                            preferred_element_type=jnp.float32,
                        )
                        for n in range(cols // BLOCK)
                    ],
                    axis=1,
                )
            )
        input_gate = jax.nn.sigmoid(mapped[0])
        recur_gate = jax.nn.sigmoid(mapped[1])
        log_keep = 8.0 * recur_gate * log_decay
        feeding = jnp.sqrt(negative_expm1(2.0 * log_keep))
        state = jnp.exp(log_keep) * earlier + feeding * input_gate * convolved.astype(jnp.float32)
        state_o[l, cut(h), :] = state
        ro[l, h] = (state * jax.nn.gelu(gate_in.astype(jnp.float32))).astype(jnp.bfloat16)
        for k, peer in enumerate(dp_peers):
            send(ro.at[l, h], rg.at[l, h, d], gs.at[l, h, k], gr.at[l, h, d], "dp", peer)
        rg[l, h, d] = ro[l, h]

    def mix(l, h):
        if h == 0:
            for copy in loads[l][2]:
                copy.wait()
        for k, peer in enumerate(dp_peers):
            arrived(rg.at[l, h, peer], gs.at[l, h, k], gr.at[l, h, peer], "dp", peer)
        readout = rg[l, h].reshape(nd * r, cols)
        mixed = jnp.dot(readout, wo_v[l], preferred_element_type=jnp.float32)
        for j in range(nt):
            mx[l, h, j] = mixed[:, j * own : (j + 1) * own].astype(jnp.bfloat16)
        for k, peer in enumerate(tp_peers):
            send(mx.at[l, h, peer], ms.at[l, h, t], ms_s.at[l, h, k], ms_r.at[l, h, t], "tp", peer)

    def collect(l, h):
        total = mx[l, h, t].astype(jnp.float32)
        total = total + xg[l, t, :, cut(h), :].reshape(nd * r, own).astype(jnp.float32)
        for k, peer in enumerate(tp_peers):
            arrived(ms.at[l, h, peer], ms_s.at[l, h, k], ms_r.at[l, h, peer], "tp", peer)
            total = total + ms[l, h, peer].astype(jnp.float32)
        result = total.astype(jnp.bfloat16).reshape(nd, r, own)
        if l + 1 < layers:
            xg[l + 1, t, :, cut(h), :] = result
            send_features(l + 1, h)
        else:
            mix_o[:, cut(h), :] = result

    stores = []

    def store(src, dst):
        copy = pltpu.make_async_copy(src, dst, out_sem.at[len(stores)])
        copy.start()
        stores.append(copy)

    c_stream.wait()
    pl.semaphore_wait(barrier, nt - 1 + nd - 1)
    for h in range(halves):
        send_features(0, h)
    for l in range(layers):
        for h in range(halves):
            project(l, h)
        for h in range(halves):
            recur(l, h)
        for h in range(halves):
            mix(l, h)
        store(state_o.at[l], new_state.at[l])
        store(win_o.at[l], new_window.at[l])
        for h in range(halves):
            collect(l, h)
    store(mix_o, mixed_out)
    for copy in sends:
        copy.wait_send()
    for copy in stores:
        copy.wait()


def fused(
    nt,
    nd,
    halves,
    stream,
    lengths,
    prior_state,
    prior_window,
    norm_gain,
    w_branch,
    w_gate_branch,
    conv_taps,
    w_in_gate,
    w_rec_gate,
    decay_param,
    w_out,
):
    layers, width, cols = w_branch.shape
    batch, own = stream.shape
    rows = batch // nd
    r = rows // halves
    depth = prior_window.shape[2]
    window = prior_window.transpose(0, 2, 1, 3)
    bf16, f32 = jnp.bfloat16, jnp.float32
    anywhere = pl.BlockSpec(memory_space=pl.ANY)
    dma = pltpu.SemaphoreType.DMA
    mixed, state, new_window = pl.pallas_call(
        functools.partial(fused_kernel, nt, nd, halves),
        out_shape=(
            jax.ShapeDtypeStruct((nd, rows, own), bf16),
            jax.ShapeDtypeStruct(prior_state.shape, f32),
            jax.ShapeDtypeStruct(window.shape, bf16),
        ),
        in_specs=[anywhere] * 12,
        out_specs=(anywhere,) * 3,
        scratch_shapes=[
            pltpu.VMEM((layers, nt, nd, rows, own), bf16),
            pltpu.VMEM((layers, halves, nd, r, 2 * cols + 128), bf16),
            pltpu.VMEM((layers, halves, nd, r, 2 * cols + 128), bf16),
            pltpu.VMEM((layers, halves, r, cols), bf16),
            pltpu.VMEM((layers, halves, nd, r, cols), bf16),
            pltpu.VMEM((layers, halves, nt, nd * r, own), bf16),
            pltpu.VMEM((layers, halves, nt, nd * r, own), bf16),
            pltpu.VMEM((1, rows), jnp.int32),
            pltpu.VMEM(prior_state.shape, f32),
            pltpu.VMEM(window.shape, bf16),
            pltpu.VMEM(norm_gain.shape, f32),
            pltpu.VMEM((layers, 2, width, cols), bf16),
            pltpu.VMEM(conv_taps.shape, bf16),
            pltpu.VMEM((layers, 2, BLOCK, cols), bf16),
            pltpu.VMEM(decay_param.shape, f32),
            pltpu.VMEM(w_out.shape, bf16),
            pltpu.VMEM(prior_state.shape, f32),
            pltpu.VMEM(window.shape, bf16),
            pltpu.VMEM((nd, rows, own), bf16),
            dma((5 + 7 * layers,)),
            dma((2 * layers + 1,)),
            dma((layers, halves, nt)),
            dma((layers, halves, nt)),
            dma((layers, halves, nd)),
            dma((layers, halves, nd)),
            dma((layers, halves, nd)),
            dma((layers, halves, nd)),
            dma((layers, halves, nt)),
            dma((layers, halves, nt)),
        ],
        compiler_params=pltpu.CompilerParams(collective_id=0, has_side_effects=True),
    )(
        stream.reshape(nd, rows, own),
        lengths.reshape(1, rows),
        prior_state,
        window,
        norm_gain,
        w_branch,
        w_gate_branch,
        conv_taps,
        w_in_gate,
        w_rec_gate,
        decay_param,
        w_out,
    )
    return mixed.reshape(batch, own), state, new_window.transpose(0, 2, 1, 3)


def step(nt, nd, *arrays):
    stream, w_branch = arrays[0], arrays[5]
    rows, cols = stream.shape[0] // nd, w_branch.shape[2]
    if cols % BLOCK == 0 and stream.shape[1] % 128 == 0 and rows % (16 * HALVES) == 0:
        return fused(nt, nd, HALVES, *arrays)
    return body(*arrays)


def solution(mesh):
    placed = (
        P(None, ("dp", "tp")),
        P("dp"),
        P(None, "dp", "tp"),
        P(None, "dp", None, "tp"),
        P(None, "dp"),
        P(None, "dp", "tp"),
        P(None, "dp", "tp"),
        P(None, None, "tp"),
        P(None, None, "tp"),
        P(None, None, "tp"),
        P(None, "tp"),
        P(None, "tp", "dp"),
    )
    return jax.shard_map(
        functools.partial(step, mesh.shape["tp"], mesh.shape["dp"]),
        mesh=mesh,
        in_specs=placed,
        out_specs=(P(None, ("dp", "tp")), P(None, "dp", "tp"), P(None, "dp", None, "tp")),
        check_vma=False,
    )
```

```python
import functools

import jax
import jax.numpy as jnp
from jax import lax
from jax.experimental import pallas as pl
from jax.experimental.pallas import tpu as pltpu
from jax.sharding import PartitionSpec as P

D = 4096
BLOCK = 256


epsilon = 1e-06


def from_partner(block, axis, apart):
    count = lax.axis_size(axis)
    route = []
    for low in range(count):
        high = low | 1 << apart
        if high != low and high < count:
            route += [(low, high), (high, low)]
    return lax.ppermute(block, axis, route)


def norm_rows(block_rows, gain_values, squares):
    scaling = lax.rsqrt(squares / D + epsilon)
    return (block_rows.astype(jnp.float32) * scaling * gain_values).astype(jnp.bfloat16)


def normed_input(stream_local, gain_block):
    own_width = stream_local.shape[1]
    offset = lax.axis_index("tp") * own_width
    widened = stream_local.astype(jnp.float32)
    squares = lax.psum(jnp.sum(widened * widened, axis=1, keepdims=True), ("tp", "dp"))
    own_gain = lax.dynamic_slice_in_dim(gain_block, offset, own_width, 0)
    result = lax.all_gather(norm_rows(stream_local, own_gain, squares), "tp", axis=1, tiled=True)
    return result


def peer_block(convolved):
    col_count = convolved.shape[1]
    group_size = max(BLOCK // col_count, 1)
    device = lax.axis_index("tp")
    grouped = convolved
    for bit_number in range(group_size.bit_length() - 1):
        partner = from_partner(grouped, "tp", bit_number)
        is_upper = device // (1 << bit_number) % 2 == 1
        grouped = jnp.where(
            is_upper,
            jnp.concatenate([partner, grouped], axis=1),
            jnp.concatenate([grouped, partner], axis=1),
        )
    return grouped


def block_gates(grouped, weight):
    row_count = grouped.shape[0]
    col_count = weight.shape[1]
    blocks = max(col_count // BLOCK, 1)
    block_cols = min(col_count, BLOCK)
    inputs = grouped.reshape(row_count, blocks, BLOCK)
    tables = weight.reshape(BLOCK, blocks, block_cols)
    mapped = jnp.einsum("rnk,knc->rnc", inputs, tables, preferred_element_type=jnp.float32)
    return mapped.reshape(row_count, col_count)


def recurrent_step(
    normed,
    lengths,
    prior_state,
    prior_window,
    w_branch,
    w_gate_branch,
    conv_taps,
    w_in_gate,
    w_rec_gate,
    decay_param,
    w_out,
    stream_local,
):
    col_count = w_branch.shape[1]
    summed = lax.psum_scatter(
        jnp.concatenate(
            [
                jnp.dot(normed, w_branch, preferred_element_type=jnp.float32),
                jnp.dot(normed, w_gate_branch, preferred_element_type=jnp.float32),
            ],
            axis=1,
        ).astype(jnp.bfloat16),
        "dp",
        scatter_dimension=0,
        tiled=True,
    ).astype(jnp.float32)
    branch = summed[:, :col_count].astype(jnp.bfloat16)
    gate_in = summed[:, col_count:].astype(jnp.bfloat16)
    depth = prior_window.shape[1]
    needed = depth + 1 - jnp.arange(depth, dtype=jnp.int32)
    living = lengths[:, None, None] >= needed[None, :, None]
    history = jnp.where(living, prior_window, jnp.zeros_like(prior_window))
    window = jnp.concatenate([history, branch[:, None, :]], axis=1)
    convolved = jnp.sum(
        window.astype(jnp.float32) * conv_taps.astype(jnp.float32)[None], axis=1
    ).astype(jnp.bfloat16)
    grouped = peer_block(convolved)
    input_gate = jax.nn.sigmoid(block_gates(grouped, w_in_gate))
    recur_gate = jax.nn.sigmoid(block_gates(grouped, w_rec_gate))
    log_keep = 8.0 * recur_gate * jax.nn.log_sigmoid(decay_param)
    keeping = jnp.exp(log_keep)
    feeding = jnp.sqrt(-jnp.expm1(2.0 * log_keep))
    earlier = jnp.where(lengths[:, None] >= 2, prior_state, jnp.zeros_like(prior_state))
    state = keeping * earlier + feeding * input_gate * convolved.astype(jnp.float32)
    readout = (state * jax.nn.gelu(gate_in.astype(jnp.float32))).astype(jnp.bfloat16)
    mixed = jnp.dot(
        lax.all_gather(readout, "dp", axis=0, tiled=True), w_out, preferred_element_type=jnp.float32
    )
    own_width = stream_local.shape[1]
    offset = lax.axis_index("tp") * own_width
    own_cols = lax.dynamic_slice_in_dim(mixed, offset, own_width, 1) + stream_local.astype(
        jnp.float32
    )
    terms = lax.dynamic_update_slice_in_dim(mixed, own_cols, offset, 1)
    return (terms, state, window[:, 1:])


def body(
    stream,
    lengths,
    prior_state,
    prior_window,
    norm_gain,
    w_branch,
    w_gate_branch,
    conv_taps,
    w_in_gate,
    w_rec_gate,
    decay_param,
    w_out,
):
    normed = normed_input(stream, norm_gain[0])
    terms, state_first, window_first = recurrent_step(
        normed,
        lengths,
        prior_state[0],
        prior_window[0],
        w_branch[0],
        w_gate_branch[0],
        conv_taps[0],
        w_in_gate[0],
        w_rec_gate[0],
        decay_param[0],
        w_out[0],
        stream,
    )
    carried = lax.psum(terms, "tp").astype(jnp.bfloat16)
    widened = carried.astype(jnp.float32)
    squares = lax.psum(jnp.sum(widened * widened, axis=1, keepdims=True), "dp")
    normed = norm_rows(carried, norm_gain[1], squares)
    own_width = stream.shape[1]
    first = lax.dynamic_slice_in_dim(carried, lax.axis_index("tp") * own_width, own_width, 1)
    terms, state_second, window_second = recurrent_step(
        normed,
        lengths,
        prior_state[1],
        prior_window[1],
        w_branch[1],
        w_gate_branch[1],
        conv_taps[1],
        w_in_gate[1],
        w_rec_gate[1],
        decay_param[1],
        w_out[1],
        first,
    )
    second = lax.psum_scatter(terms, "tp", scatter_dimension=1, tiled=True).astype(jnp.bfloat16)
    return (
        second,
        jnp.stack([state_first, state_second]),
        jnp.stack([window_first, window_second]),
    )


HALVES = 4
MAIN_VMEM = 60 * 1024 * 1024
TAIL_VMEM = 4 * 1024 * 1024
MESH = pl.DeviceIdType.MESH


def negative_expm1(z):
    series = -z * (1.0 + z / 2.0 * (1.0 + z / 3.0 * (1.0 + z / 4.0 * (1.0 + z / 5.0))))
    return jnp.where(z > -0.1, series, 1.0 - jnp.exp(z))


def fused_kernel(
    nt,
    nd,
    halves,
    stream,
    lengths,
    prior_state,
    prior_window,
    norm_gain,
    w_branch,
    w_gate_branch,
    conv_taps,
    w_in_gate,
    w_rec_gate,
    decay_param,
    w_out,
    mixed_out,
    new_state,
    new_window,
    xg,
    part,
    pr,
    ro,
    rg,
    mx,
    ms,
    len_v,
    state_v,
    win_v,
    gain_v,
    wp_v,
    taps_v,
    gates_v,
    decay_v,
    wo_v,
    state_o,
    win_o,
    mix_o,
    in_sem,
    out_sem,
    xs,
    xr,
    ps,
    prs,
    gs,
    gr,
    ms_s,
    ms_r,
):
    t = lax.axis_index("tp")
    d = lax.axis_index("dp")
    layers = w_branch.shape[0]
    rows, own = stream.shape[1], stream.shape[2]
    r = rows // halves
    cols = w_branch.shape[2]
    width = w_branch.shape[1]

    barrier = pltpu.get_barrier_semaphore()
    tp_peers = [lax.rem(t + k, nt) for k in range(1, nt)]
    dp_peers = [lax.rem(d + k, nd) for k in range(1, nd)]
    for peer in tp_peers:
        pl.semaphore_signal(barrier, inc=1, device_id={"tp": peer}, device_id_type=MESH)
    for peer in dp_peers:
        pl.semaphore_signal(barrier, inc=1, device_id={"dp": peer}, device_id_type=MESH)

    counter = [0]

    def load(src, dst):
        copy = pltpu.make_async_copy(src, dst, in_sem.at[counter[0]])
        counter[0] += 1
        copy.start()
        return copy

    c_stream = load(stream, xg.at[0, t])
    c_gain = load(norm_gain, gain_v)
    c_len = load(lengths, len_v)
    loads = []
    for l in range(layers):
        c_w = [load(w_branch.at[l], wp_v.at[l, 0]), load(w_gate_branch.at[l], wp_v.at[l, 1])]
        c_s = [
            load(prior_window.at[l], win_v.at[l]),
            load(prior_state.at[l], state_v.at[l]),
            load(w_in_gate.at[l], gates_v.at[l, 0]),
            load(w_rec_gate.at[l], gates_v.at[l, 1]),
        ]
        if l == 0:
            c_s += [load(conv_taps, taps_v), load(decay_param, decay_v), c_len]
        c_o = [load(w_out.at[l], wo_v.at[l])]
        loads.append((c_w, c_s, c_o))

    sends = []

    def send(src, dst, ssem, rsem, axis, peer):
        copy = pltpu.make_async_remote_copy(
            src_ref=src,
            dst_ref=dst,
            send_sem=ssem,
            recv_sem=rsem,
            device_id={axis: peer},
            device_id_type=MESH,
        )
        copy.start()
        sends.append(copy)

    def arrived(dst, ssem, rsem, axis, peer):
        pltpu.make_async_remote_copy(
            src_ref=dst,
            dst_ref=dst,
            send_sem=ssem,
            recv_sem=rsem,
            device_id={axis: peer},
            device_id_type=MESH,
        ).wait_recv()

    def cut(h):
        return slice(h * r, (h + 1) * r)

    def send_features(l, h):
        for k, peer in enumerate(tp_peers):
            block = xg.at[l, t, :, pl.ds(h * r, r), :]
            send(block, block, xs.at[l, h, k], xr.at[l, h, t], "tp", peer)

    def project(l, h):
        for k, peer in enumerate(tp_peers):
            block = xg.at[l, peer, :, pl.ds(h * r, r), :]
            arrived(block, xs.at[l, h, k], xr.at[l, h, peer], "tp", peer)
        if h == 0:
            if l == 0:
                c_gain.wait()
            for copy in loads[l][0]:
                copy.wait()
        squares = jnp.zeros((nd * r, own), jnp.float32)
        pieces = []
        for j in range(nt):
            x = xg[l, j, :, cut(h), :].reshape(nd * r, own).astype(jnp.float32)
            squares = squares + x * x
            gain = gain_v[l : l + 1, j * own : (j + 1) * own]
            pieces.append((x * gain).astype(jnp.bfloat16))
        normed = jnp.concatenate(pieces, axis=1)
        total = jnp.sum(squares, axis=1, keepdims=True)
        high = total.astype(jnp.bfloat16).astype(jnp.float32)
        lane = lax.broadcasted_iota(jnp.int32, (nd * r, 128), 1)
        both = jnp.where(lane < 64, high, total - high).astype(jnp.bfloat16)
        part[l, h, :, :, 2 * cols :] = both.reshape(nd, r, 128)
        for w in range(2):
            product = jnp.dot(normed, wp_v[l, w], preferred_element_type=jnp.float32)
            part[l, h, :, :, w * cols : (w + 1) * cols] = product.astype(jnp.bfloat16).reshape(
                nd, r, cols
            )
        for k, peer in enumerate(dp_peers):
            send(
                part.at[l, h, peer],
                pr.at[l, h, d],
                ps.at[l, h, k],
                prs.at[l, h, d],
                "dp",
                peer,
            )

    def recur(l, h):
        summed = part[l, h, d].astype(jnp.float32)
        if h == 0:
            for copy in loads[l][1]:
                copy.wait()
        length = jnp.sum(
            jnp.where(
                lax.broadcasted_iota(jnp.int32, (r, rows), 0) + h * r
                == lax.broadcasted_iota(jnp.int32, (r, rows), 1),
                jnp.broadcast_to(len_v[...].astype(jnp.float32), (r, rows)),
                0.0,
            ),
            axis=1,
            keepdims=True,
        )
        depth = prior_window.shape[1]
        history = []
        for m in range(depth):
            row = win_v[l, m, cut(h), :].astype(jnp.float32)
            history.append(jnp.where(length >= depth + 1 - m, row, 0.0))
        taps = taps_v[l].astype(jnp.float32)
        before = history[0] * taps[0:1]
        for m in range(1, depth):
            before = before + history[m] * taps[m : m + 1]
        raw = decay_v[l : l + 1]
        log_decay = jnp.minimum(raw, 0.0) - jnp.log1p(jnp.exp(-jnp.abs(raw)))
        earlier = jnp.where(length >= 2, state_v[l, cut(h), :], 0.0)

        for k, peer in enumerate(dp_peers):
            arrived(pr.at[l, h, peer], ps.at[l, h, k], prs.at[l, h, peer], "dp", peer)
        for peer in dp_peers:
            summed = summed + pr[l, h, peer].astype(jnp.float32)
        squares = summed[:, 2 * cols : 2 * cols + 1] + summed[:, 2 * cols + 64 : 2 * cols + 65]
        scaling = lax.rsqrt(squares / (width * nd) + epsilon)
        branch = (summed[:, :cols] * scaling).astype(jnp.bfloat16)
        gate_in = (summed[:, cols : 2 * cols] * scaling).astype(jnp.bfloat16)
        for m in range(1, depth):
            win_o[l, m - 1, cut(h), :] = history[m].astype(jnp.bfloat16)
        win_o[l, depth - 1, cut(h), :] = branch
        convolved = (before + branch.astype(jnp.float32) * taps[depth : depth + 1]).astype(
            jnp.bfloat16
        )
        mapped = []
        for w in range(2):
            mapped.append(
                jnp.concatenate(
                    [
                        jnp.dot(
                            convolved[:, n * BLOCK : (n + 1) * BLOCK],
                            gates_v[l, w, :, n * BLOCK : (n + 1) * BLOCK],
                            preferred_element_type=jnp.float32,
                        )
                        for n in range(cols // BLOCK)
                    ],
                    axis=1,
                )
            )
        input_gate = jax.nn.sigmoid(mapped[0])
        recur_gate = jax.nn.sigmoid(mapped[1])
        log_keep = 8.0 * recur_gate * log_decay
        feeding = jnp.sqrt(negative_expm1(2.0 * log_keep))
        state = jnp.exp(log_keep) * earlier + feeding * input_gate * convolved.astype(jnp.float32)
        state_o[l, cut(h), :] = state
        ro[l, h] = (state * jax.nn.gelu(gate_in.astype(jnp.float32))).astype(jnp.bfloat16)
        for k, peer in enumerate(dp_peers):
            send(ro.at[l, h], rg.at[l, h, d], gs.at[l, h, k], gr.at[l, h, d], "dp", peer)
        rg[l, h, d] = ro[l, h]

    def mix(l, h):
        if h == 0:
            for copy in loads[l][2]:
                copy.wait()
        for k, peer in enumerate(dp_peers):
            arrived(rg.at[l, h, peer], gs.at[l, h, k], gr.at[l, h, peer], "dp", peer)
        readout = rg[l, h].reshape(nd * r, cols)
        mixed = jnp.dot(readout, wo_v[l], preferred_element_type=jnp.float32)
        for j in range(nt):
            mx[l, h, j] = mixed[:, j * own : (j + 1) * own].astype(jnp.bfloat16)
        for k, peer in enumerate(tp_peers):
            send(mx.at[l, h, peer], ms.at[l, h, t], ms_s.at[l, h, k], ms_r.at[l, h, t], "tp", peer)

    def collect(l, h):
        total = mx[l, h, t].astype(jnp.float32)
        total = total + xg[l, t, :, cut(h), :].reshape(nd * r, own).astype(jnp.float32)
        for k, peer in enumerate(tp_peers):
            arrived(ms.at[l, h, peer], ms_s.at[l, h, k], ms_r.at[l, h, peer], "tp", peer)
            total = total + ms[l, h, peer].astype(jnp.float32)
        result = total.astype(jnp.bfloat16).reshape(nd, r, own)
        if l + 1 < layers:
            xg[l + 1, t, :, cut(h), :] = result
            send_features(l + 1, h)
        else:
            mix_o[:, cut(h), :] = result

    stores = []

    def store(src, dst):
        copy = pltpu.make_async_copy(src, dst, out_sem.at[len(stores)])
        copy.start()
        stores.append(copy)

    c_stream.wait()
    pl.semaphore_wait(barrier, nt - 1 + nd - 1)
    for h in range(halves):
        send_features(0, h)
    for l in range(layers):
        for h in range(halves):
            project(l, h)
        for h in range(halves):
            recur(l, h)
        for h in range(halves):
            mix(l, h)
        store(state_o.at[l], new_state.at[l])
        store(win_o.at[l], new_window.at[l])
        for h in range(halves):
            collect(l, h)
    store(mix_o, mixed_out)
    for copy in sends:
        copy.wait_send()
    for copy in stores:
        copy.wait()


def tail_kernel(mixed, state, window, mixed_out, state_out, window_out, a, b, c, in_sem, out_sem):
    triples = ((mixed, a, mixed_out), (state, b, state_out), (window, c, window_out))
    loads = []
    for k, (src, held, _) in enumerate(triples):
        loads.append(pltpu.make_async_copy(src, held, in_sem.at[k]))
        loads[-1].start()
    stores = []
    for k, (_, held, dst) in enumerate(triples):
        loads[k].wait()
        stores.append(pltpu.make_async_copy(held, dst, out_sem.at[k]))
        stores[-1].start()
    for copy in stores:
        copy.wait()


def fused(
    nt,
    nd,
    halves,
    stream,
    lengths,
    prior_state,
    prior_window,
    norm_gain,
    w_branch,
    w_gate_branch,
    conv_taps,
    w_in_gate,
    w_rec_gate,
    decay_param,
    w_out,
):
    layers, width, cols = w_branch.shape
    batch, own = stream.shape
    rows = batch // nd
    r = rows // halves
    depth = prior_window.shape[2]
    window = prior_window.transpose(0, 2, 1, 3)
    bf16, f32 = jnp.bfloat16, jnp.float32
    anywhere = pl.BlockSpec(memory_space=pl.ANY)
    dma = pltpu.SemaphoreType.DMA
    mixed, state, new_window = pl.pallas_call(
        functools.partial(fused_kernel, nt, nd, halves),
        out_shape=(
            jax.ShapeDtypeStruct((nd, rows, own), bf16),
            jax.ShapeDtypeStruct(prior_state.shape, f32),
            jax.ShapeDtypeStruct(window.shape, bf16),
        ),
        in_specs=[pl.BlockSpec(memory_space=pltpu.HBM)] * 12,
        out_specs=(anywhere,) * 3,
        scratch_shapes=[
            pltpu.VMEM((layers, nt, nd, rows, own), bf16),
            pltpu.VMEM((layers, halves, nd, r, 2 * cols + 128), bf16),
            pltpu.VMEM((layers, halves, nd, r, 2 * cols + 128), bf16),
            pltpu.VMEM((layers, halves, r, cols), bf16),
            pltpu.VMEM((layers, halves, nd, r, cols), bf16),
            pltpu.VMEM((layers, halves, nt, nd * r, own), bf16),
            pltpu.VMEM((layers, halves, nt, nd * r, own), bf16),
            pltpu.VMEM((1, rows), jnp.int32),
            pltpu.VMEM(prior_state.shape, f32),
            pltpu.VMEM(window.shape, bf16),
            pltpu.VMEM(norm_gain.shape, f32),
            pltpu.VMEM((layers, 2, width, cols), bf16),
            pltpu.VMEM(conv_taps.shape, bf16),
            pltpu.VMEM((layers, 2, BLOCK, cols), bf16),
            pltpu.VMEM(decay_param.shape, f32),
            pltpu.VMEM(w_out.shape, bf16),
            pltpu.VMEM(prior_state.shape, f32),
            pltpu.VMEM(window.shape, bf16),
            pltpu.VMEM((nd, rows, own), bf16),
            dma((5 + 7 * layers,)),
            dma((2 * layers + 1,)),
            dma((layers, halves, nt)),
            dma((layers, halves, nt)),
            dma((layers, halves, nd)),
            dma((layers, halves, nd)),
            dma((layers, halves, nd)),
            dma((layers, halves, nd)),
            dma((layers, halves, nt)),
            dma((layers, halves, nt)),
        ],
        compiler_params=pltpu.CompilerParams(collective_id=0, has_side_effects=True, vmem_limit_bytes=MAIN_VMEM),
    )(
        stream.reshape(nd, rows, own),
        lengths.reshape(1, rows),
        prior_state,
        window,
        norm_gain,
        w_branch,
        w_gate_branch,
        conv_taps,
        w_in_gate,
        w_rec_gate,
        decay_param,
        w_out,
    )
    finals = (mixed, state, new_window)
    mixed, state, new_window = pl.pallas_call(
        tail_kernel,
        out_shape=tuple(jax.ShapeDtypeStruct(a.shape, a.dtype) for a in finals),
        in_specs=[anywhere] * 3,
        out_specs=(anywhere,) * 3,
        scratch_shapes=[pltpu.VMEM(a.shape, a.dtype) for a in finals] + [dma((3,)), dma((3,))],
        compiler_params=pltpu.CompilerParams(vmem_limit_bytes=TAIL_VMEM),
    )(*finals)
    return mixed.reshape(batch, own), state, new_window.transpose(0, 2, 1, 3)


def step(nt, nd, *arrays):
    stream, w_branch = arrays[0], arrays[5]
    rows, cols = stream.shape[0] // nd, w_branch.shape[2]
    if cols % BLOCK == 0 and stream.shape[1] % 128 == 0 and rows % (8 * HALVES) == 0:
        return fused(nt, nd, HALVES, *arrays)
    return body(*arrays)


def solution(mesh):
    placed = (
        P(None, ("dp", "tp")),
        P("dp"),
        P(None, "dp", "tp"),
        P(None, "dp", None, "tp"),
        P(None, "dp"),
        P(None, "dp", "tp"),
        P(None, "dp", "tp"),
        P(None, None, "tp"),
        P(None, None, "tp"),
        P(None, None, "tp"),
        P(None, "tp"),
        P(None, "tp", "dp"),
    )
    return jax.shard_map(
        functools.partial(step, mesh.shape["tp"], mesh.shape["dp"]),
        mesh=mesh,
        in_specs=placed,
        out_specs=(P(None, ("dp", "tp")), P(None, "dp", "tp"), P(None, "dp", None, "tp")),
        check_vma=False,
    )
```
